32 devices in a mesh: row: 8 (over z, y), col: 4 (over x, core).
Axes of the slice: x: 2, y: 2, z: 4, core: 2. Of those that a mesh axis runs over, the one named last changes fastest.
Arguments:
- tokens: bfloat16 [4096, 2048], P('row'), may hold values from -6 to 6
- outer_weight: bfloat16 [2048, 1024], P(None, 'col'), may hold values from -0.125 to 0.125
- inner_weight: bfloat16 [2048, 1024], P(None, 'col'), may hold values from -0.125 to 0.125
- value_weight: bfloat16 [2048, 1024], P(None, 'col'), may hold values from -0.125 to 0.125
- conv_taps: float32 [3, 3, 1024], P(None, None, 'col'), may hold values from -3.5 to 3.5
- feature_weight: float32 [33, 128], replicated, may hold values from -1 to 1
- feature_phase: float32 [128], replicated, may hold values from -3.140625 to 3.140625
- inner_mats: float32 [2, 128, 128], replicated, may hold values from -0.5 to 0.5
- inner_phase: float32 [2, 128], replicated, may hold values from -3.140625 to 3.140625
- frequency: float32 [128], replicated, may hold values from 0.1 to 1.9
- forward_weight: float32 [128, 1024], P(None, 'col'), may hold values from -0.5 to 0.5
- backward_weight: float32 [128, 1024], P(None, 'col'), may hold values from -0.5 to 0.5
- decay_rate: float32 [1024], P('col'), may hold values from 0.2 to 409.6, as said below
- skip_gain: float32 [1024], P('col'), may hold values from -6 to 6
- output_weight: bfloat16 [1024, 2048], replicated, may hold values from -0.1875 to 0.1875
Outputs:
- layer_out: bfloat16 [4096, 2048], P(('row', 'col'))
The draws below stay inside these ranges and needn't reach their ends.
Inputs may be any that keep to these rules, and one draw needn't show every extreme that they name: `decay_rate`: positive rates of the channels' filter windows.
All inputs are finite; a program needn't handle non-finite values.
Results may differ from the reference program's by a relative error of at most 0.014.
Values may be sent and summed in bfloat16 or wider, within the bound.
A program may use at most 64 MiB of HBM per device.

```python
import math
import jax
import jax.numpy as jnp
from jax import lax

D = 2048
C = 1024
UNITS = 128
BANDS = 16
INNER = 2
LENGTH = 4096


def draw_decay_rate(key, part):
    picker, slow_key, fast_key = jax.random.split(key, 3)
    share = 0.5
    fast_mask = jax.random.uniform(picker, (C,), jnp.float32) < share
    slow_rate = jax.random.uniform(slow_key, (C,), jnp.float32, 0.2, 2.0)
    fast_rate = LENGTH / jax.random.uniform(fast_key, (C,), jnp.float32, 10.0, 30.0)
    return jnp.where(fast_mask, fast_rate, slow_rate).astype(jnp.float32)


def block_scale(own_key, shape, shards, least, largest):
    gain = 1.0
    for position, parts in shards:
        heights = jax.random.uniform(jax.random.fold_in(jax.random.fold_in(own_key, 6), position), (parts,), jnp.float32, least / len(shards), largest / len(shards))
        gain = gain * jnp.repeat(jnp.exp(heights), shape[position] // parts).reshape((-1,) + (1,) * (len(shape) - 1 - position))
    return gain


def centred(own_key, shape, width, limit, cuts=(), kind=jnp.bfloat16):
    values = jax.random.normal(own_key, shape, jnp.float32) * width
    if len(cuts) > 0:
        values = block_scale(own_key, shape, cuts, -0.22, 0.18) * values
    return jnp.clip(values, min=-limit, max=limit).astype(kind)


def setup_inputs(seed: int = 0) -> dict:
    arg_keys = jax.random.split(jax.random.key(seed), 16)
    tokens = centred(arg_keys[0], (LENGTH, D), 1.0, 6.0, ((0, 8),))
    outer_weight = centred(arg_keys[1], (D, C), D ** -0.5, 0.125, ((1, 4),))
    inner_weight = centred(arg_keys[2], (D, C), D ** -0.5, 0.125, ((1, 4),))
    value_weight = centred(arg_keys[3], (D, C), D ** -0.5, 0.125, ((1, 4),))
    conv_taps = centred(arg_keys[4], (3, 3, C), 0.577, 3.5, ((2, 4),), jnp.float32)
    feature_weight = centred(arg_keys[5], (2 * BANDS + 1, UNITS), (2 * BANDS + 1) ** -0.5, 1.0, (), jnp.float32)
    feature_phase = jnp.clip(jax.random.uniform(arg_keys[6], (UNITS,), jnp.float32, -3.140625, 3.140625), -3.140625, 3.140625)
    inner_mats = centred(arg_keys[7], (INNER, UNITS, UNITS), UNITS ** -0.5, 0.5, (), jnp.float32)
    inner_phase = jnp.clip(jax.random.uniform(arg_keys[8], (INNER, UNITS), jnp.float32, -3.140625, 3.140625), -3.140625, 3.140625)
    frequency = jnp.clip(1.0 + 0.18 * jax.random.normal(arg_keys[9], (UNITS,), jnp.float32), 0.1, 1.9)
    forward_weight = centred(arg_keys[10], (UNITS, C), UNITS ** -0.5, 0.5, ((1, 4),), jnp.float32)
    backward_weight = centred(arg_keys[11], (UNITS, C), UNITS ** -0.5, 0.5, ((1, 4),), jnp.float32)
    decay_rate = draw_decay_rate(jax.random.fold_in(arg_keys[15], 71), 0)
    skip_gain = centred(arg_keys[13], (C,), 1.0, 6.0, ((0, 4),), jnp.float32)
    output_weight = centred(arg_keys[14], (C, D), C ** -0.5, 0.1875)
    return {"tokens": tokens, "outer_weight": outer_weight, "inner_weight": inner_weight, "value_weight": value_weight, "conv_taps": conv_taps, "feature_weight": feature_weight, "feature_phase": feature_phase, "inner_mats": inner_mats, "inner_phase": inner_phase, "frequency": frequency, "forward_weight": forward_weight, "backward_weight": backward_weight, "decay_rate": decay_rate, "skip_gain": skip_gain, "output_weight": output_weight}


PRECISE = lax.Precision.HIGHEST

def short_conv(projected, tap_rows):
    padded = jnp.pad(projected.astype(jnp.float32), ((1, 1), (0, 0)))
    return padded[:-2] * tap_rows[0] + padded[1:-1] * tap_rows[1] + padded[2:] * tap_rows[2]

def reference(tokens, outer_weight, inner_weight, value_weight, conv_taps, feature_weight, feature_phase, inner_mats, inner_phase, frequency, forward_weight, backward_weight, decay_rate, skip_gain, output_weight):
    outer_proj = jnp.dot(tokens, outer_weight, preferred_element_type=jnp.float32).astype(jnp.bfloat16)
    inner_proj = jnp.dot(tokens, inner_weight, preferred_element_type=jnp.float32).astype(jnp.bfloat16)
    value_proj = jnp.dot(tokens, value_weight, preferred_element_type=jnp.float32).astype(jnp.bfloat16)
    places = jnp.arange(LENGTH, dtype=jnp.int32)
    scaled = places.astype(jnp.float32) / (LENGTH - 1)
    band_ints = 1 + jnp.arange(BANDS, dtype=jnp.int32) * (LENGTH // (4 * BANDS))
    turns = places[:, None] * band_ints[None, :] % LENGTH
    angles = 2.0 * math.pi / LENGTH * turns.astype(jnp.float32)
    features = jnp.concatenate([scaled[:, None], jnp.cos(angles), -jnp.sin(angles)], axis=1)
    hidden = jnp.sin(frequency * (jnp.dot(features, feature_weight, precision=PRECISE) + feature_phase))
    for level_index in range(INNER):
        hidden = jnp.sin(frequency * (jnp.dot(hidden, inner_mats[level_index], precision=PRECISE) + inner_phase[level_index]))
    channel_block = 128
    block_count = C // channel_block

    def split_cols(matrix):
        return matrix.reshape(matrix.shape[0], block_count, channel_block).transpose(1, 0, 2)

    def one_block(pieces):
        outer_part, inner_part, value_part, tap_block, ahead_cols, behind_cols, rates, skips = pieces
        gate_part = short_conv(outer_part, tap_block[:, 0]).astype(jnp.bfloat16)
        signal = (short_conv(inner_part, tap_block[:, 1]) * short_conv(value_part, tap_block[:, 2])).astype(jnp.bfloat16)
        window = jnp.exp(-scaled[:, None] * rates[None, :])
        filter_ahead = jnp.dot(hidden, ahead_cols, precision=PRECISE) * window
        filter_behind = jnp.dot(hidden, behind_cols, precision=PRECISE) * window
        norm_scale = lax.rsqrt(1.0 + lax.optimization_barrier(jnp.sum(jnp.square(filter_ahead), axis=0)) + lax.optimization_barrier(jnp.sum(jnp.square(filter_behind[1:]), axis=0)))
        kernel = jnp.concatenate([filter_ahead, jnp.zeros((1, channel_block), jnp.float32), filter_behind[:0:-1]], axis=0) * norm_scale
        signal_wide = signal.astype(jnp.float32)
        spectrum = jnp.fft.rfft(signal_wide, n=2 * LENGTH, axis=0) * jnp.fft.rfft(kernel, axis=0)
        response = jnp.fft.irfft(spectrum, n=2 * LENGTH, axis=0)[:LENGTH].astype(jnp.bfloat16)
        response = lax.optimization_barrier(response)
        return (gate_part.astype(jnp.float32) * (response.astype(jnp.float32) + skips * signal_wide)).astype(jnp.bfloat16)
    taps_split = conv_taps.reshape(3, 3, block_count, channel_block).transpose(2, 0, 1, 3)
    mixed_blocks = lax.map(one_block, (split_cols(outer_proj), split_cols(inner_proj), split_cols(value_proj), taps_split, split_cols(forward_weight), split_cols(backward_weight), decay_rate.reshape(block_count, channel_block), skip_gain.reshape(block_count, channel_block)))
    mixed_rows = mixed_blocks.transpose(1, 0, 2).reshape(LENGTH, C)
    return jnp.dot(mixed_rows, output_weight, preferred_element_type=jnp.float32).astype(jnp.bfloat16)
```

```python
import functools
import math

import jax
import jax.numpy as jnp
import numpy as np
from jax import lax
from jax.experimental import pallas as pl
from jax.experimental.pallas import tpu as pltpu
from jax.sharding import PartitionSpec as P

BANDS = 16
INNER = 2
FACTOR = 256


PRECISE = lax.Precision.HIGHEST


def with_halo(array, sides, width):
    for axis, dim in sides:
        devices, length = (lax.axis_size(axis), array.shape[dim])
        up = [(i, (i + 1) % devices) for i in range(devices - 1)]
        down = [(j, i) for i, j in up]
        last = lax.slice_in_dim(array, length - width, length, axis=dim)
        leading = lax.slice_in_dim(array, 0, width, axis=dim)
        before = lax.ppermute(last, axis, up)
        after = lax.ppermute(leading, axis, down)
        array = jnp.concatenate([before, array, after], axis=dim)
    return array


def phases(height, breadth, period):
    row_index = lax.broadcasted_iota(jnp.int32, (height, breadth), 0)
    col_index = lax.broadcasted_iota(jnp.int32, (height, breadth), 1)
    phase_angle = 2.0 * math.pi / period * (row_index * col_index % period).astype(jnp.float32)
    return (jnp.cos(phase_angle), jnp.sin(phase_angle))


def along_last(operand, matrix):
    return jnp.einsum("ckb,bj->ckj", operand, matrix, precision=PRECISE)


def forward_transform(operand, tables):
    cosine_one, sine_one, twist_cos, twist_sin, cosine_two, sine_two = tables
    used_rows = operand.shape[1]
    first_real = jnp.einsum("kr,crb->ckb", cosine_one[:, :used_rows], operand, precision=PRECISE)
    first_imag = -jnp.einsum("kr,crb->ckb", sine_one[:, :used_rows], operand, precision=PRECISE)
    turned_real = first_real * twist_cos + first_imag * twist_sin
    turned_imag = first_imag * twist_cos - first_real * twist_sin
    spec_real = along_last(turned_real, cosine_two) + along_last(turned_imag, sine_two)
    spec_imag = along_last(turned_imag, cosine_two) - along_last(turned_real, sine_two)
    return (spec_real, spec_imag)


def inverse_transform(spec_real, spec_imag, tables, kept_rows):
    cosine_one, sine_one, twist_cos, twist_sin, cosine_two, sine_two = tables
    back_real = along_last(spec_real, cosine_two) - along_last(spec_imag, sine_two)
    back_imag = along_last(spec_imag, cosine_two) + along_last(spec_real, sine_two)
    untwist_real = back_real * twist_cos - back_imag * twist_sin
    untwist_imag = back_imag * twist_cos + back_real * twist_sin
    return jnp.einsum(
        "nk,ckb->cnb", cosine_one[:kept_rows], untwist_real, precision=PRECISE
    ) - jnp.einsum("nk,ckb->cnb", sine_one[:kept_rows], untwist_imag, precision=PRECISE)


def position_filters(
    places,
    seq_length,
    feature_weight,
    feature_phase,
    inner_mats,
    inner_phase,
    frequency,
    forward_cols,
    backward_cols,
    rates,
):
    scaled = places.astype(jnp.float32) / (seq_length - 1)
    band_ints = 1 + jnp.arange(BANDS, dtype=jnp.int32) * (seq_length // (4 * BANDS))
    turns = places[:, None] * band_ints[None, :] % seq_length
    angles = 2.0 * math.pi / seq_length * turns.astype(jnp.float32)
    features = jnp.concatenate([scaled[:, None], jnp.cos(angles), -jnp.sin(angles)], axis=1)
    hidden = jnp.sin(
        frequency * (jnp.dot(features, feature_weight, precision=PRECISE) + feature_phase)
    )
    for level_index in range(INNER):
        hidden = jnp.sin(
            frequency
            * (
                jnp.dot(hidden, inner_mats[level_index], precision=PRECISE)
                + inner_phase[level_index]
            )
        )
    window = jnp.exp(-scaled[:, None] * rates[None, :])
    filter_ahead = jnp.dot(hidden, forward_cols, precision=PRECISE) * window
    filter_behind = jnp.dot(hidden, backward_cols, precision=PRECISE) * window
    return (filter_ahead, filter_behind)


def on_device(
    tokens,
    outer_weight,
    inner_weight,
    value_weight,
    conv_taps,
    feature_weight,
    feature_phase,
    inner_mats,
    inner_phase,
    frequency,
    forward_weight,
    backward_weight,
    decay_rate,
    skip_gain,
    output_weight,
):
    block_rows = tokens.shape[0]
    seq_length = block_rows * lax.axis_size("row")
    own_width = outer_weight.shape[1]
    outer_proj = jnp.dot(tokens, outer_weight, preferred_element_type=jnp.float32).astype(
        jnp.bfloat16
    )
    inner_proj = jnp.dot(tokens, inner_weight, preferred_element_type=jnp.float32).astype(
        jnp.bfloat16
    )
    value_proj = jnp.dot(tokens, value_weight, preferred_element_type=jnp.float32).astype(
        jnp.bfloat16
    )
    stacked = jnp.concatenate([outer_proj, inner_proj, value_proj], axis=1)
    padded = with_halo(stacked, (("row", 0),), 1).astype(jnp.float32)
    tap_table = conv_taps.reshape(3, 3 * own_width)
    convolved = padded[:-2] * tap_table[0] + padded[1:-1] * tap_table[1] + padded[2:] * tap_table[2]
    gate_part = convolved[:, :own_width].astype(jnp.bfloat16)
    signal = (convolved[:, own_width : 2 * own_width] * convolved[:, 2 * own_width :]).astype(
        jnp.bfloat16
    )
    offset = lax.axis_index("row") * block_rows
    places = offset + jnp.arange(block_rows, dtype=jnp.int32)
    filter_ahead, filter_behind = position_filters(
        places,
        seq_length,
        feature_weight,
        feature_phase,
        inner_mats,
        inner_phase,
        frequency,
        forward_weight,
        backward_weight,
        decay_rate,
    )
    moved_signal, moved_ahead, moved_behind = (
        lax.all_to_all(signal.astype(jnp.float32), "row", split_axis=1, concat_axis=0, tiled=True),
        lax.all_to_all(filter_ahead, "row", split_axis=1, concat_axis=0, tiled=True),
        lax.all_to_all(filter_behind, "row", split_axis=1, concat_axis=0, tiled=True),
    )
    per_device = moved_ahead.shape[1]
    ahead_rows = moved_ahead.T
    behind_rows = moved_behind.T
    norm_scale = lax.rsqrt(
        1.0
        + jnp.sum(jnp.square(ahead_rows), axis=1)
        + jnp.sum(jnp.square(behind_rows[:, 1:]), axis=1)
    )
    kernel_rows = (
        jnp.concatenate(
            [ahead_rows, jnp.zeros((per_device, 1), jnp.float32), jnp.flip(behind_rows[:, 1:], 1)],
            axis=1,
        )
        * norm_scale[:, None]
    )
    padded_length = 2 * seq_length
    height = padded_length // FACTOR
    tables = (
        phases(height, height, height)
        + phases(height, FACTOR, padded_length)
        + phases(FACTOR, FACTOR, FACTOR)
    )
    kernel_real, kernel_imag = forward_transform(
        kernel_rows.reshape(per_device, height, FACTOR), tables
    )
    signal_real, signal_imag = forward_transform(
        moved_signal.T.reshape(per_device, height // 2, FACTOR), tables
    )
    prod_real = signal_real * kernel_real - signal_imag * kernel_imag
    prod_imag = signal_real * kernel_imag + signal_imag * kernel_real
    response = inverse_transform(prod_real, prod_imag, tables, height // 2) / padded_length
    response = response.reshape(per_device, seq_length).T.astype(jnp.bfloat16)
    returned = lax.all_to_all(response, "row", split_axis=0, concat_axis=1, tiled=True)
    mixed_rows = (
        gate_part.astype(jnp.float32)
        * (returned.astype(jnp.float32) + skip_gain * signal.astype(jnp.float32))
    ).astype(jnp.bfloat16)
    whole_rows = lax.all_to_all(mixed_rows, "col", split_axis=0, concat_axis=1, tiled=True)
    return jnp.dot(whole_rows, output_weight, preferred_element_type=jnp.float32).astype(
        jnp.bfloat16
    )


WIDE = 256


def feature_table(seq_length):
    places = np.arange(seq_length, dtype=np.int64)
    bands = 1 + np.arange(BANDS, dtype=np.int64) * (seq_length // (4 * BANDS))
    angles = 2.0 * np.pi / seq_length * (places[:, None] * bands[None, :] % seq_length)
    scaled = places / (seq_length - 1)
    feats = np.concatenate([scaled[:, None], np.cos(angles), -np.sin(angles)], 1).astype(np.float32)
    high = feats.astype(jnp.bfloat16)
    low = (feats - high.astype(np.float32)).astype(jnp.bfloat16)
    used = np.zeros((seq_length, 128), jnp.bfloat16)
    count = feats.shape[1]
    for start, part in ((0, high), (40, low), (80, high)):
        used[:, start : start + count] = part
    used[:, 120:122] = 1
    return used


def sine_coefficients():
    u = 0.5 * np.cos(np.pi * (np.arange(4000) + 0.5) / 8000)
    powers = np.stack([u ** (2 * i + 1) for i in range(6)], 1)
    return [float(v) for v in np.linalg.lstsq(powers, np.sin(2 * np.pi * u), rcond=None)[0]]


SINE = sine_coefficients()
MAGIC = 12582912.0


def sine_of_turns(turns):
    u = turns - ((turns + MAGIC) - MAGIC)
    square = u * u
    total = SINE[-1]
    for value in SINE[-2::-1]:
        total = total * square + value
    return u * total


def split_two(value):
    high = value.astype(jnp.bfloat16)
    return high, (value - high.astype(jnp.float32)).astype(jnp.bfloat16)


def combine(terms):
    total = None
    for coef, array in terms:
        if abs(coef) < 1e-9:
            continue
        if abs(abs(coef) - 1.0) < 1e-9:
            if total is None:
                total = array if coef > 0 else -array
            else:
                total = total + array if coef > 0 else total - array
        else:
            total = array * coef if total is None else total + array * coef
    return total


def first_stage(planes):
    half = len(planes)
    full, mid = 2 * half, half // 2
    quarter = mid // 2
    theta = 2 * math.pi / full
    add = {r: planes[r] + planes[half - r] for r in range(1, mid)}
    sub = {r: planes[r] - planes[half - r] for r in range(1, mid)}
    add_add = {r: add[r] + add[mid - r] for r in range(1, quarter)}
    add_sub = {r: add[r] - add[mid - r] for r in range(1, quarter)}
    sub_add = {r: sub[r] + sub[mid - r] for r in range(1, quarter)}
    sub_sub = {r: sub[r] - sub[mid - r] for r in range(1, quarter)}
    ends = (planes[0] + planes[mid], planes[0] - planes[mid])
    out = []
    for k in range(half + 1):
        cos = lambda r: math.cos(theta * r * k)
        sin = lambda r: math.sin(theta * r * k)
        if k % 4 == 0:
            real = combine([(1.0, ends[0]), (cos(quarter), add[quarter])] + [(cos(r), add_add[r]) for r in add_add])
            imag = combine([(-sin(r), sub_sub[r]) for r in sub_sub])
        elif k % 2 == 0:
            real = combine([(1.0, ends[1])] + [(cos(r), add_sub[r]) for r in add_sub])
            imag = combine([(-sin(quarter), sub[quarter])] + [(-sin(r), sub_add[r]) for r in sub_add])
        else:
            real = combine([(1.0, planes[0])] + [(cos(r), sub[r]) for r in sub])
            imag = combine([(-sin(mid), planes[mid])] + [(-sin(r), add[r]) for r in add])
        out.append((real, imag))
    return out


def last_stage(pairs):
    half = len(pairs) - 1
    full, mid = 2 * half, half // 2
    quarter = mid // 2
    theta = 2 * math.pi / full
    four = range(0, half + 1, 4)
    two = range(2, half + 1, 4)
    odd = range(1, half + 1, 2)
    real = [p[0] for p in pairs]
    imag = [p[1] for p in pairs]
    out = [None] * half

    def cosines(r, ks):
        return combine([(math.cos(theta * r * k), real[k]) for k in ks])

    def sines(r, ks):
        return combine([(math.sin(theta * r * k), imag[k]) for k in ks])

    out[0] = combine([(1.0, v) for v in real])
    out[mid] = cosines(mid, list(four) + list(two)) - sines(mid, odd)

    def place(r, cos_even, sin_even):
        cos_odd, sin_odd = cosines(r, odd), sines(r, odd)
        out[r] = (cos_even - sin_even) + (cos_odd - sin_odd)
        out[half - r] = (cos_even + sin_even) - (cos_odd + sin_odd)

    for r in range(1, quarter):
        c0, c2, s0, s2 = cosines(r, four), cosines(r, two), sines(r, four), sines(r, two)
        place(r, c0 + c2, s0 + s2)
        place(mid - r, c0 - c2, s2 - s0)
    place(quarter, cosines(quarter, four), sines(quarter, two))
    return out


GROUP = 16
LANES = 128
CHUNK = 512


def layer_kernel(
    tokens_h, outer_h, inner_h, value_h, feats_h, output_h,
    taps_h, feature_weight_h, feature_phase_h, inner_mats_h, inner_phase_h, frequency_h, forward_h, backward_h,
    rate_h, skip_h, twist_h, trig_h,
    out_ref,
    tok, weights, outer_w, feats, output_w, taps, feature_weight, feature_phase, inner_mats, inner_phase, frequency,
    forward, backward, rate, skip, twist, trig,
    hid, sig_send, sig_recv, gs_send, gs_recv, resp_send, resp_recv,
    sums, diffs, turned, filt, back, scale_ref, first_ref, chan, rate_col, energy_ref, proj_ref, signal_ref, total_ref,
    edge_ref, edge_out, edge_in, end_ref,
    load_sem, small_sem, edge_send, edge_recv, hid_s, hid_r, sig_s, sig_r, gs_s, gs_r, resp_s, resp_r,
):
    f32, bf16 = jnp.float32, jnp.bfloat16
    dot = functools.partial(jnp.dot, preferred_element_type=f32)
    n_row, n_col = lax.axis_size("row"), lax.axis_size("col")
    row, col = lax.axis_index("row"), lax.axis_index("col")
    rows, depth = tokens_h.shape
    length = rows * n_row
    half = feats.shape[0]
    width = outer_h.shape[1]
    count = width // n_row
    parts = count // GROUP
    wide = width // parts
    planes = length // WIDE
    per = rows // WIDE
    share = rows // n_col
    spec = (planes + 1) * GROUP
    mesh_id = pl.DeviceIdType.MESH

    barrier = pltpu.get_barrier_semaphore()
    for o in range(1, n_row):
        pl.semaphore_signal(barrier, inc=1, device_id=(lax.rem(row + o, n_row), col), device_id_type=mesh_id)
    for o in range(1, n_col):
        pl.semaphore_signal(barrier, inc=1, device_id=(row, lax.rem(col + o, n_col)), device_id_type=mesh_id)
    side = lax.rem(col, 2)
    partner = col + 1 - 2 * side
    small = [
        pltpu.make_async_copy(source, target, small_sem.at[i])
        for i, (source, target) in enumerate([
            (feature_weight_h, feature_weight), (feature_phase_h, feature_phase), (inner_mats_h, inner_mats),
            (inner_phase_h, inner_phase), (frequency_h, frequency), (forward_h, forward), (backward_h, backward),
            (rate_h, rate), (taps_h, taps), (skip_h, skip), (twist_h, twist), (trig_h, trig)])
    ]
    feature_load = pltpu.make_async_copy(
        feats_h.at[pl.ds(pl.multiple_of(side * half, CHUNK), half)], feats, load_sem.at[0])
    first_load = pltpu.make_async_copy(tokens_h.at[0:16], tok.at[0:16], load_sem.at[1])
    last_load = pltpu.make_async_copy(tokens_h.at[rows - 16 : rows], tok.at[rows - 16 : rows], load_sem.at[2])
    token_load = pltpu.make_async_copy(tokens_h.at[16 : rows - 16], tok.at[16 : rows - 16], load_sem.at[3])
    weight_loads = [
        [
            pltpu.make_async_copy(
                source.at[:, h * wide : (h + 1) * wide], weights.at[h, :, j * wide : (j + 1) * wide],
                load_sem.at[4 + 2 * h + j])
            for j, source in enumerate((inner_h, value_h))
        ]
        for h in range(parts)
    ]
    base = 4 + 2 * parts
    outer_load = pltpu.make_async_copy(outer_h, outer_w, load_sem.at[base])
    output_loads = [
        pltpu.make_async_copy(
            output_h.at[c * width + h * wide : c * width + (h + 1) * wide],
            output_w.at[h, c * wide : (c + 1) * wide], load_sem.at[base + 1 + h * n_col + c])
        for h in range(parts) for c in range(n_col)
    ]
    for copy in small[:5] + [feature_load, first_load, last_load, token_load]:
        copy.start()
    for pair in weight_loads:
        for copy in pair:
            copy.start()
    for copy in small[5:]:
        copy.start()

    for copy in small[:5]:
        copy.wait()
    turn = frequency[...] * (0.5 / math.pi)
    high, low = split_two(feature_weight[...] * turn)
    phase_high, phase_low = split_two(feature_phase[...] * turn)
    used = high.shape[0]
    first_ref[...] = jnp.zeros_like(first_ref)
    first_ref[0:used] = high.astype(f32)
    first_ref[40 : 40 + used] = high.astype(f32)
    first_ref[80 : 80 + used] = low.astype(f32)
    first_ref[120:121] = phase_high.astype(f32)
    first_ref[121:122] = phase_low.astype(f32)
    first_w = first_ref[...].astype(bf16)
    inner_w = []
    for level in range(INNER):
        mat_high, mat_low = split_two(inner_mats[level] * turn)
        inner_w.append(jnp.concatenate([
            jnp.concatenate([mat_high, mat_low], 1), jnp.concatenate([mat_high, jnp.zeros_like(mat_low)], 1)], 0))
    inner_p = inner_phase[...] * turn

    def hidden_chunk(i):
        at = pl.ds(i * CHUNK, CHUNK)
        hidden = sine_of_turns(dot(feats[at, :], first_w))
        for level in range(INNER):
            h_high, h_low = split_two(hidden)
            both = dot(jnp.concatenate([h_high, h_low], 1), inner_w[level])
            hidden = sine_of_turns(both[:, :LANES] + both[:, LANES:] + inner_p[level : level + 1, :])
        hid[side, at, :] = hidden.astype(bf16)

    pieces = half // CHUNK
    to_partner = []
    for i in range(pieces):
        part = hid.at[side, pl.ds(i * CHUNK, CHUNK)]
        to_partner.append(pltpu.make_async_remote_copy(
            src_ref=part, dst_ref=part, send_sem=hid_s.at[i], recv_sem=hid_r.at[i],
            device_id=(row, partner), device_id_type=mesh_id))

    feature_load.wait()
    for i in range(pieces // 2):
        hidden_chunk(i)
    pl.semaphore_wait(barrier, n_row + n_col - 2)
    first_load.wait()
    last_load.wait()
    ends = [tok[rows - 16 : rows].astype(f32)[15:16], tok[0:16].astype(f32)[0:1]]
    for j, end in enumerate(ends):
        for i in range(depth // LANES):
            edge_ref[j, i : i + 1, :] = end[:, i * LANES : (i + 1) * LANES]
        edge_out[j] = edge_ref[j].astype(bf16)
    down = pltpu.make_async_remote_copy(
        src_ref=edge_out.at[0], dst_ref=edge_in.at[0],
        send_sem=edge_send.at[0], recv_sem=edge_recv.at[0],
        device_id=(lax.rem(row + 1, n_row), col), device_id_type=mesh_id)
    up = pltpu.make_async_remote_copy(
        src_ref=edge_out.at[1], dst_ref=edge_in.at[1],
        send_sem=edge_send.at[1], recv_sem=edge_recv.at[1],
        device_id=(lax.rem(row + n_row - 1, n_row), col), device_id_type=mesh_id)

    @pl.when(row < n_row - 1)
    def _():
        down.start()

    @pl.when(row > 0)
    def _():
        up.start()

    for i in range(pieces // 2):
        to_partner[i].start()

    token_load.wait()
    for pair in weight_loads:
        for copy in pair:
            copy.wait()
    for copy in [outer_load] + output_loads:
        copy.start()
    for h in range(parts):
        proj_ref[h] = dot(tok[...], weights[h]).astype(bf16)

    for copy in small[5:]:
        copy.wait()
    chan[0] = forward[...].T
    chan[1] = backward[...].T
    rate_col[...] = jnp.broadcast_to(rate[...], (LANES, width)).T
    mine = [pl.ds(pl.multiple_of(h * wide + row * GROUP, GROUP), GROUP) for h in range(parts)]
    both_w = jnp.concatenate([chan[j, own, :] for j in range(2) for own in mine], 0).astype(bf16)
    rates = jnp.concatenate([rate_col[own, 0:1] for own in mine], 0)
    energy_ref[...] = jnp.zeros_like(energy_ref)

    @pl.when(row > 0)
    def _():
        down.wait_recv()

    @pl.when(row < n_row - 1)
    def _():
        up.wait_recv()

    for j in range(2):
        edge_ref[j] = edge_in[j].astype(f32)
        for i in range(depth // LANES):
            end_ref[j : j + 1, i * LANES : (i + 1) * LANES] = edge_ref[j, i : i + 1, :]
    end_rows = end_ref[...].astype(bf16)

    index = lax.broadcasted_iota(jnp.int32, (rows, 2 * wide), 0)

    def convolved(main, ends, tap):
        first = jnp.where(row > 0, ends[0:1], 0.0)
        last = jnp.where(row < n_row - 1, ends[1:2], 0.0)
        at_row = index[:, : main.shape[1]]
        before = jnp.where(at_row == 0, first, pltpu.roll(main, 1, 0))
        after = jnp.where(at_row == rows - 1, last, pltpu.roll(main, rows - 1, 0))
        return before * tap[0] + main * tap[1] + after * tap[2]

    def rounded(value):
        return value.astype(bf16).astype(f32)

    other = 1 - lax.div(row, n_row // 2)
    place = lax.rem(row, n_row // 2)
    peers = [other * (n_row // 2) + lax.rem(place + i, n_row // 2) for i in range(n_row // 2)]
    peers += [(1 - other) * (n_row // 2) + lax.rem(place + i, n_row // 2) for i in range(1, n_row // 2)]

    sig_copies = []
    for h in range(parts):
        ends = rounded(dot(end_rows, weights[h]))
        at = slice(h * wide, (h + 1) * wide)
        tap = [jnp.concatenate([taps[i, 1:2, at], taps[i, 2:3, at]], 1) for i in range(3)]
        made = convolved(proj_ref[h].astype(f32), ends, tap)
        signal = (made[:, :wide] * made[:, wide:]).astype(bf16).astype(f32).T
        signal_ref[h] = signal
        flipped = signal.astype(bf16)
        for g in range(n_row):
            sig_send[h, g] = flipped[g * GROUP : (g + 1) * GROUP]
        for i, peer in enumerate(peers):
            sig_copies.append(pltpu.make_async_remote_copy(
                src_ref=sig_send.at[h, peer], dst_ref=sig_recv.at[h, row],
                send_sem=sig_s.at[h, i], recv_sem=sig_r.at[h, i],
                device_id=(peer, col), device_id_type=mesh_id))
            sig_copies[-1].start()
        sig_recv[h, row] = sig_send[h, row]

    outer_load.wait()
    skip_col = jnp.broadcast_to(skip[...], (LANES, width)).T
    for h in range(parts):
        at = slice(h * wide, (h + 1) * wide)
        main = rounded(dot(tok[...], outer_w[:, at]))
        ends = rounded(dot(end_rows, outer_w[:, at]))
        gate = rounded(convolved(main, ends, [taps[i, 0:1, at] for i in range(3)])).T.astype(bf16)
        direct = (signal_ref[h] * skip_col[at, 0:1]).astype(bf16)
        for p in range(n_col):
            gs_send[p, 0, h] = gate[:, p * share : (p + 1) * share]
            gs_send[p, 1, h] = direct[:, p * share : (p + 1) * share]
    gs_copies = []
    for o in range(1, n_col):
        peer = lax.rem(col + o, n_col)
        gs_copies.append(pltpu.make_async_remote_copy(
            src_ref=gs_send.at[peer], dst_ref=gs_recv.at[col],
            send_sem=gs_s.at[o], recv_sem=gs_r.at[o], device_id=(row, peer), device_id_type=mesh_id))
        gs_copies[-1].start()
    gs_recv[col] = gs_send[col]

    for i in range(pieces // 2, pieces):
        hidden_chunk(i)
        to_partner[i].start()

    def filter_chunk(owner, i):
        start = owner * half + i * CHUNK
        at = pl.ds(pl.multiple_of(start, CHUNK), CHUNK)
        both = lax.dot_general(both_w, hid[owner, pl.ds(i * CHUNK, CHUNK), :], (((1,), (1,)), ((), ())),
                               preferred_element_type=f32)
        place = lax.broadcasted_iota(jnp.int32, (count, CHUNK), 1) + start
        window = jnp.exp(place.astype(f32) * (-1.0 / (length - 1)) * rates)
        ahead = both[:count] * window
        behind = jnp.where(place == 0, 0.0, both[count:] * window)
        sums[:, at] = ahead + behind
        diffs[:, at] = ahead - behind
        energy_ref[...] += jnp.broadcast_to(
            jnp.sum(ahead * ahead + behind * behind, axis=1, keepdims=True), (count, LANES))

    for i in range(pieces):
        filter_chunk(side, i)
    for i in range(pieces):
        to_partner[i].wait_recv()
        filter_chunk(1 - side, i)
    scale_ref[...] = lax.rsqrt(1.0 + energy_ref[...]) * (0.5 / length)

    def turn_into(first, pairs, base_row, left, weighted):
        for k, (real, imag) in enumerate(pairs):
            c, s = twist[0, k : k + 1, pl.ds(left, LANES)], twist[1, k : k + 1, pl.ds(left, LANES)]
            if weighted and k not in (0, planes):
                c, s = c * 2.0, s * 2.0
            at = pl.ds(pl.multiple_of(base_row + k * GROUP, GROUP), GROUP)
            if imag is None:
                new_real, new_imag = real * c, -(real * s)
            else:
                new_real, new_imag = real * c + imag * s, imag * c - real * s
            turned[first, at, pl.ds(left, LANES)] = new_real.astype(bf16)
            turned[first, at, pl.ds(pl.multiple_of(WIDE + left, LANES), LANES)] = new_imag.astype(bf16)

    lanes = WIDE // LANES

    def filter_tile(i, carry):
        h, left = i // lanes, pl.multiple_of(i % lanes * LANES, LANES)
        top = pl.ds(pl.multiple_of(h * GROUP, GROUP), GROUP)
        scale = scale_ref[top, :]
        for which, source in enumerate((sums, diffs)):
            got = [source[top, pl.ds(pl.multiple_of(r * WIDE + left, LANES), LANES)] * scale for r in range(planes)]
            turn_into(which, first_stage(got), h * spec, left, True)
        return carry

    lax.fori_loop(0, parts * lanes, filter_tile, 0)
    filt[0] = dot(turned[0], trig[:, :WIDE])
    filt[1] = dot(turned[1], trig[:, WIDE:])

    resp_copies = []
    for h in range(parts):
        for copy in sig_copies[h * (n_row - 1) : (h + 1) * (n_row - 1)]:
            copy.wait_recv()
        band = pl.ds(h * spec, spec)

        def signal_tile(i, carry):
            left = pl.multiple_of(i * LANES, LANES)
            got = [sig_recv[h, r // per, :, pl.ds(pl.multiple_of(r % per * WIDE + left, LANES), LANES)].astype(f32)
                   for r in range(planes)]
            turn_into(0, first_stage(got), h * spec, left, False)
            return carry

        lax.fori_loop(0, lanes, signal_tile, 0)
        spectrum = dot(turned[0, band], trig[...])
        real, imag = spectrum[:, :WIDE], spectrum[:, WIDE:]
        prod_real = (real * filt[0, band] - imag * filt[1, band]).astype(bf16)
        prod_imag = (real * filt[1, band] + imag * filt[0, band]).astype(bf16)
        back[...] = dot(jnp.concatenate([prod_imag, prod_real], 1), trig[...])

        def back_tile(i, carry):
            left = pl.multiple_of(i * LANES, LANES)
            pairs = []
            for k in range(planes + 1):
                c, s = twist[0, k : k + 1, pl.ds(left, LANES)], twist[1, k : k + 1, pl.ds(left, LANES)]
                at = pl.ds(k * GROUP, GROUP)
                b_imag, b_real = back[at, pl.ds(left, LANES)], back[at, pl.ds(pl.multiple_of(WIDE + left, LANES), LANES)]
                pairs.append((b_real * c - b_imag * s, b_imag * c + b_real * s))
            for r, plane in enumerate(last_stage(pairs)):
                resp_send[h, r // per, r % per * lanes + i] = plane.astype(bf16)
            return carry

        lax.fori_loop(0, lanes, back_tile, 0)
        for i, peer in enumerate(peers + [row]):
            for o in range(n_col):
                if i == n_row - 1 and o == 0:
                    continue
                target = lax.rem(col + o, n_col)
                resp_copies.append(pltpu.make_async_remote_copy(
                    src_ref=resp_send.at[h, peer, target], dst_ref=resp_recv.at[h, col, row],
                    send_sem=resp_s.at[h], recv_sem=resp_r.at[h, col],
                    device_id=(peer, target), device_id_type=mesh_id))
                resp_copies[-1].start()
        resp_recv[h, col, row] = resp_send[h, row, col]

    for copy in gs_copies:
        copy.wait_recv()
    for copy in output_loads:
        copy.wait()
    for h in range(parts):
        for o in range(n_col):
            source = lax.rem(col + o, n_col)
            come = resp_recv.at[h, source, pl.ds(0, n_row - 1 if o == 0 else n_row)]
            pltpu.make_async_copy(come, come, resp_r.at[h, source]).wait()
        shape = (n_col * wide, share)
        response = resp_recv[h].reshape(shape).astype(f32)
        gate, direct = (gs_recv[:, j, h].reshape(shape).astype(f32) for j in range(2))
        mixed = (gate * (response + direct)).T.astype(bf16)
        got = dot(mixed, output_w[h])
        if h == 0:
            total_ref[...] = got
        elif h < parts - 1:
            total_ref[...] += got
        else:
            out_ref[...] = (total_ref[...] + got).astype(bf16)

    @pl.when(row < n_row - 1)
    def _():
        down.wait_send()

    @pl.when(row > 0)
    def _():
        up.wait_send()

    for copy in to_partner + sig_copies + gs_copies:
        copy.wait_send()
    for h in range(parts):
        gone = resp_send.at[h].reshape(n_row * n_col, GROUP, share).at[pl.ds(0, n_row * n_col - 1)]
        pltpu.make_async_copy(gone, gone, resp_s.at[h]).wait()


def fits(tokens_rows, seq_length, own_width, row_devices, col_devices, units):
    planes = seq_length // WIDE
    members = own_width // row_devices
    return (
        members % (2 * GROUP) == 0
        and own_width % row_devices == 0
        and row_devices * GROUP % LANES == 0
        and row_devices % 2 == 0
        and tokens_rows % WIDE == 0
        and planes % 8 == 0
        and 8 <= planes <= 32
        and units == LANES
        and col_devices == 4
        and tokens_rows == col_devices * LANES
        and seq_length % (4 * CHUNK) == 0
    )


def on_device_fast(
    tokens, outer_weight, inner_weight, value_weight, conv_taps, feature_weight, feature_phase,
    inner_mats, inner_phase, frequency, forward_weight, backward_weight, decay_rate, skip_gain, output_weight,
):
    f32, bf16 = jnp.float32, jnp.bfloat16
    rows, depth = tokens.shape
    devices = lax.axis_size("row")
    seq_length = rows * devices
    width = outer_weight.shape[1]
    members = width // devices
    parts = members // GROUP
    wide = width // parts
    planes = seq_length // WIDE
    n_col = lax.axis_size("col")
    k_index = np.arange(planes + 1)[:, None] * np.arange(WIDE)[None, :]
    twist_angle = 2 * np.pi * k_index / (2 * seq_length)
    twist = jnp.asarray(np.stack([np.cos(twist_angle), np.sin(twist_angle)]), f32)
    w_angle = 2 * np.pi * (np.arange(WIDE)[:, None] * np.arange(WIDE)[None, :] % WIDE) / WIDE
    cos_w, sin_w = np.cos(w_angle), np.sin(w_angle)
    trig = jnp.asarray(np.block([[cos_w, -sin_w], [sin_w, cos_w]]), bf16)
    spec = (planes + 1) * GROUP
    any_spec = pl.BlockSpec(memory_space=pl.ANY)
    vmem = pl.BlockSpec(memory_space=pltpu.VMEM)
    dma = pltpu.SemaphoreType.DMA
    share = rows // n_col
    half = seq_length // 2
    pieces = half // CHUNK
    small = [
        conv_taps, feature_weight, feature_phase[None], inner_mats, inner_phase, frequency[None],
        forward_weight, backward_weight, decay_rate[None], skip_gain[None], twist, trig]
    exchanged = pltpu.VMEM((parts, devices, GROUP, rows), bf16)
    spread = pltpu.VMEM((n_col, 2, parts, wide, share), bf16)
    return pl.pallas_call(
        layer_kernel,
        out_shape=pltpu.VMEM((share, output_weight.shape[1]), bf16),
        in_specs=[any_spec] * (6 + len(small)),
        out_specs=vmem,
        scratch_shapes=[
            pltpu.VMEM((rows, depth), bf16),
            pltpu.VMEM((parts, depth, 2 * wide), bf16),
            pltpu.VMEM((depth, width), bf16),
            pltpu.VMEM((half, LANES), bf16),
            pltpu.VMEM((parts, n_col * wide, output_weight.shape[1]), bf16),
        ] + [pltpu.VMEM(a.shape, a.dtype) for a in small] + [
            pltpu.VMEM((2, half, LANES), bf16),
            exchanged, exchanged, spread, spread,
            pltpu.VMEM((parts, devices, n_col, GROUP, share), bf16),
            pltpu.VMEM((parts, n_col, devices, GROUP, share), bf16),
            pltpu.VMEM((members, seq_length), f32),
            pltpu.VMEM((members, seq_length), f32),
            pltpu.VMEM((2, parts * spec, 2 * WIDE), bf16),
            pltpu.VMEM((2, parts * spec, WIDE), f32),
            pltpu.VMEM((spec, 2 * WIDE), f32),
            pltpu.VMEM((members, LANES), f32),
            pltpu.VMEM((LANES, LANES), f32),
            pltpu.VMEM((2, width, LANES), f32),
            pltpu.VMEM((width, LANES), f32),
            pltpu.VMEM((members, LANES), f32),
            pltpu.VMEM((parts, rows, 2 * wide), bf16),
            pltpu.VMEM((parts, wide, rows), f32),
            pltpu.VMEM((share, output_weight.shape[1]), f32),
            pltpu.VMEM((2, depth // LANES, LANES), f32),
            pltpu.VMEM((2, depth // LANES, LANES), bf16),
            pltpu.VMEM((2, depth // LANES, LANES), bf16),
            pltpu.VMEM((16, depth), f32),
            dma((5 + 2 * parts + parts * n_col,)), dma((len(small),)), dma((2,)), dma((2,)), dma((pieces,)), dma((pieces,)),
            dma((parts, devices)), dma((parts, devices)), dma((n_col,)), dma((n_col,)), dma((parts,)), dma((parts, n_col)),
        ],
        compiler_params=pltpu.CompilerParams(
            collective_id=0, has_side_effects=True, vmem_limit_bytes=GRANT),
        name="layer",
    )(tokens, outer_weight, inner_weight, value_weight, jnp.asarray(feature_table(seq_length)), output_weight, *small)


GRANT = 58 * 1024 * 1024


def on_any(*args):
    tokens, outer_weight, feature_weight = args[0], args[1], args[5]
    devices = lax.axis_size("row")
    if fits(tokens.shape[0], tokens.shape[0] * devices, outer_weight.shape[1], devices, lax.axis_size("col"), feature_weight.shape[1]):
        return on_device_fast(*args)
    return on_device(*args)


def solution(mesh):
    placed = (
        P("row", None),
        P(None, "col"),
        P(None, "col"),
        P(None, "col"),
        P(None, None, "col"),
        P(),
        P(),
        P(),
        P(),
        P(),
        P(None, "col"),
        P(None, "col"),
        P("col"),
        P("col"),
        P(),
    )
    return jax.shard_map(
        on_any, mesh=mesh, in_specs=placed, out_specs=P(("row", "col"), None), check_vma=False
    )
```

```python
import functools
import math

import jax
import jax.numpy as jnp
import numpy as np
from jax import lax
from jax.experimental import pallas as pl
from jax.experimental.pallas import tpu as pltpu
from jax.sharding import PartitionSpec as P

BANDS = 16
INNER = 2
FACTOR = 256


PRECISE = lax.Precision.HIGHEST


def with_halo(array, sides, width):
    for axis, dim in sides:
        devices, length = (lax.axis_size(axis), array.shape[dim])
        up = [(i, (i + 1) % devices) for i in range(devices - 1)]
        down = [(j, i) for i, j in up]
        last = lax.slice_in_dim(array, length - width, length, axis=dim)
        leading = lax.slice_in_dim(array, 0, width, axis=dim)
        before = lax.ppermute(last, axis, up)
        after = lax.ppermute(leading, axis, down)
        array = jnp.concatenate([before, array, after], axis=dim)
    return array


def phases(height, breadth, period):
    row_index = lax.broadcasted_iota(jnp.int32, (height, breadth), 0)
    col_index = lax.broadcasted_iota(jnp.int32, (height, breadth), 1)
    phase_angle = 2.0 * math.pi / period * (row_index * col_index % period).astype(jnp.float32)
    return (jnp.cos(phase_angle), jnp.sin(phase_angle))


def along_last(operand, matrix):
    return jnp.einsum("ckb,bj->ckj", operand, matrix, precision=PRECISE)


def forward_transform(operand, tables):
    cosine_one, sine_one, twist_cos, twist_sin, cosine_two, sine_two = tables
    used_rows = operand.shape[1]
    first_real = jnp.einsum("kr,crb->ckb", cosine_one[:, :used_rows], operand, precision=PRECISE)
    first_imag = -jnp.einsum("kr,crb->ckb", sine_one[:, :used_rows], operand, precision=PRECISE)
    turned_real = first_real * twist_cos + first_imag * twist_sin
    turned_imag = first_imag * twist_cos - first_real * twist_sin
    spec_real = along_last(turned_real, cosine_two) + along_last(turned_imag, sine_two)
    spec_imag = along_last(turned_imag, cosine_two) - along_last(turned_real, sine_two)
    return (spec_real, spec_imag)


def inverse_transform(spec_real, spec_imag, tables, kept_rows):
    cosine_one, sine_one, twist_cos, twist_sin, cosine_two, sine_two = tables
    back_real = along_last(spec_real, cosine_two) - along_last(spec_imag, sine_two)
    back_imag = along_last(spec_imag, cosine_two) + along_last(spec_real, sine_two)
    untwist_real = back_real * twist_cos - back_imag * twist_sin
    untwist_imag = back_imag * twist_cos + back_real * twist_sin
    return jnp.einsum(
        "nk,ckb->cnb", cosine_one[:kept_rows], untwist_real, precision=PRECISE
    ) - jnp.einsum("nk,ckb->cnb", sine_one[:kept_rows], untwist_imag, precision=PRECISE)


def position_filters(
    places,
    seq_length,
    feature_weight,
    feature_phase,
    inner_mats,
    inner_phase,
    frequency,
    forward_cols,
    backward_cols,
    rates,
):
    scaled = places.astype(jnp.float32) / (seq_length - 1)
    band_ints = 1 + jnp.arange(BANDS, dtype=jnp.int32) * (seq_length // (4 * BANDS))
    turns = places[:, None] * band_ints[None, :] % seq_length
    angles = 2.0 * math.pi / seq_length * turns.astype(jnp.float32)
    features = jnp.concatenate([scaled[:, None], jnp.cos(angles), -jnp.sin(angles)], axis=1)
    hidden = jnp.sin(
        frequency * (jnp.dot(features, feature_weight, precision=PRECISE) + feature_phase)
    )
    for level_index in range(INNER):
        hidden = jnp.sin(
            frequency
            * (
                jnp.dot(hidden, inner_mats[level_index], precision=PRECISE)
                + inner_phase[level_index]
            )
        )
    window = jnp.exp(-scaled[:, None] * rates[None, :])
    filter_ahead = jnp.dot(hidden, forward_cols, precision=PRECISE) * window
    filter_behind = jnp.dot(hidden, backward_cols, precision=PRECISE) * window
    return (filter_ahead, filter_behind)


def on_device(
    tokens,
    outer_weight,
    inner_weight,
    value_weight,
    conv_taps,
    feature_weight,
    feature_phase,
    inner_mats,
    inner_phase,
    frequency,
    forward_weight,
    backward_weight,
    decay_rate,
    skip_gain,
    output_weight,
):
    block_rows = tokens.shape[0]
    seq_length = block_rows * lax.axis_size("row")
    own_width = outer_weight.shape[1]
    outer_proj = jnp.dot(tokens, outer_weight, preferred_element_type=jnp.float32).astype(
        jnp.bfloat16
    )
    inner_proj = jnp.dot(tokens, inner_weight, preferred_element_type=jnp.float32).astype(
        jnp.bfloat16
    )
    value_proj = jnp.dot(tokens, value_weight, preferred_element_type=jnp.float32).astype(
        jnp.bfloat16
    )
    stacked = jnp.concatenate([outer_proj, inner_proj, value_proj], axis=1)
    padded = with_halo(stacked, (("row", 0),), 1).astype(jnp.float32)
    tap_table = conv_taps.reshape(3, 3 * own_width)
    convolved = padded[:-2] * tap_table[0] + padded[1:-1] * tap_table[1] + padded[2:] * tap_table[2]
    gate_part = convolved[:, :own_width].astype(jnp.bfloat16)
    signal = (convolved[:, own_width : 2 * own_width] * convolved[:, 2 * own_width :]).astype(
        jnp.bfloat16
    )
    offset = lax.axis_index("row") * block_rows
    places = offset + jnp.arange(block_rows, dtype=jnp.int32)
    filter_ahead, filter_behind = position_filters(
        places,
        seq_length,
        feature_weight,
        feature_phase,
        inner_mats,
        inner_phase,
        frequency,
        forward_weight,
        backward_weight,
        decay_rate,
    )
    moved_signal, moved_ahead, moved_behind = (
        lax.all_to_all(signal.astype(jnp.float32), "row", split_axis=1, concat_axis=0, tiled=True),
        lax.all_to_all(filter_ahead, "row", split_axis=1, concat_axis=0, tiled=True),
        lax.all_to_all(filter_behind, "row", split_axis=1, concat_axis=0, tiled=True),
    )
    per_device = moved_ahead.shape[1]
    ahead_rows = moved_ahead.T
    behind_rows = moved_behind.T
    norm_scale = lax.rsqrt(
        1.0
        + jnp.sum(jnp.square(ahead_rows), axis=1)
        + jnp.sum(jnp.square(behind_rows[:, 1:]), axis=1)
    )
    kernel_rows = (
        jnp.concatenate(
            [ahead_rows, jnp.zeros((per_device, 1), jnp.float32), jnp.flip(behind_rows[:, 1:], 1)],
            axis=1,
        )
        * norm_scale[:, None]
    )
    padded_length = 2 * seq_length
    height = padded_length // FACTOR
    tables = (
        phases(height, height, height)
        + phases(height, FACTOR, padded_length)
        + phases(FACTOR, FACTOR, FACTOR)
    )
    kernel_real, kernel_imag = forward_transform(
        kernel_rows.reshape(per_device, height, FACTOR), tables
    )
    signal_real, signal_imag = forward_transform(
        moved_signal.T.reshape(per_device, height // 2, FACTOR), tables
    )
    prod_real = signal_real * kernel_real - signal_imag * kernel_imag
    prod_imag = signal_real * kernel_imag + signal_imag * kernel_real
    response = inverse_transform(prod_real, prod_imag, tables, height // 2) / padded_length
    response = response.reshape(per_device, seq_length).T.astype(jnp.bfloat16)
    returned = lax.all_to_all(response, "row", split_axis=0, concat_axis=1, tiled=True)
    mixed_rows = (
        gate_part.astype(jnp.float32)
        * (returned.astype(jnp.float32) + skip_gain * signal.astype(jnp.float32))
    ).astype(jnp.bfloat16)
    whole_rows = lax.all_to_all(mixed_rows, "col", split_axis=0, concat_axis=1, tiled=True)
    return jnp.dot(whole_rows, output_weight, preferred_element_type=jnp.float32).astype(
        jnp.bfloat16
    )


WIDE = 256


def feature_table(seq_length):
    places = np.arange(seq_length, dtype=np.int64)
    bands = 1 + np.arange(BANDS, dtype=np.int64) * (seq_length // (4 * BANDS))
    angles = 2.0 * np.pi / seq_length * (places[:, None] * bands[None, :] % seq_length)
    scaled = places / (seq_length - 1)
    feats = np.concatenate([scaled[:, None], np.cos(angles), -np.sin(angles)], 1).astype(np.float32)
    high = feats.astype(jnp.bfloat16)
    low = (feats - high.astype(np.float32)).astype(jnp.bfloat16)
    used = np.zeros((seq_length, 128), jnp.bfloat16)
    count = feats.shape[1]
    for start, part in ((0, high), (40, low), (80, high)):
        used[:, start : start + count] = part
    used[:, 120:122] = 1
    return used


def sine_coefficients():
    u = 0.5 * np.cos(np.pi * (np.arange(4000) + 0.5) / 8000)
    powers = np.stack([u ** (2 * i + 1) for i in range(6)], 1)
    return [float(v) for v in np.linalg.lstsq(powers, np.sin(2 * np.pi * u), rcond=None)[0]]


SINE = sine_coefficients()
MAGIC = 12582912.0


def sine_of_turns(turns):
    u = turns - ((turns + MAGIC) - MAGIC)
    square = u * u
    total = SINE[-1]
    for value in SINE[-2::-1]:
        total = total * square + value
    return u * total


def split_two(value):
    high = value.astype(jnp.bfloat16)
    return high, (value - high.astype(jnp.float32)).astype(jnp.bfloat16)


def combine(terms):
    total = None
    for coef, array in terms:
        if abs(coef) < 1e-9:
            continue
        if abs(abs(coef) - 1.0) < 1e-9:
            if total is None:
                total = array if coef > 0 else -array
            else:
                total = total + array if coef > 0 else total - array
        else:
            total = array * coef if total is None else total + array * coef
    return total


def first_stage(planes):
    half = len(planes)
    full, mid = 2 * half, half // 2
    quarter = mid // 2
    theta = 2 * math.pi / full
    add = {r: planes[r] + planes[half - r] for r in range(1, mid)}
    sub = {r: planes[r] - planes[half - r] for r in range(1, mid)}
    add_add = {r: add[r] + add[mid - r] for r in range(1, quarter)}
    add_sub = {r: add[r] - add[mid - r] for r in range(1, quarter)}
    sub_add = {r: sub[r] + sub[mid - r] for r in range(1, quarter)}
    sub_sub = {r: sub[r] - sub[mid - r] for r in range(1, quarter)}
    ends = (planes[0] + planes[mid], planes[0] - planes[mid])
    out = []
    for k in range(half + 1):
        cos = lambda r: math.cos(theta * r * k)
        sin = lambda r: math.sin(theta * r * k)
        if k % 4 == 0:
            real = combine([(1.0, ends[0]), (cos(quarter), add[quarter])] + [(cos(r), add_add[r]) for r in add_add])
            imag = combine([(-sin(r), sub_sub[r]) for r in sub_sub])
        elif k % 2 == 0:
            real = combine([(1.0, ends[1])] + [(cos(r), add_sub[r]) for r in add_sub])
            imag = combine([(-sin(quarter), sub[quarter])] + [(-sin(r), sub_add[r]) for r in sub_add])
        else:
            real = combine([(1.0, planes[0])] + [(cos(r), sub[r]) for r in sub])
            imag = combine([(-sin(mid), planes[mid])] + [(-sin(r), add[r]) for r in add])
        out.append((real, imag))
    return out


def last_stage(pairs):
    half = len(pairs) - 1
    full, mid = 2 * half, half // 2
    quarter = mid // 2
    theta = 2 * math.pi / full
    four = range(0, half + 1, 4)
    two = range(2, half + 1, 4)
    odd = range(1, half + 1, 2)
    real = [p[0] for p in pairs]
    imag = [p[1] for p in pairs]
    out = [None] * half

    def cosines(r, ks):
        return combine([(math.cos(theta * r * k), real[k]) for k in ks])

    def sines(r, ks):
        return combine([(math.sin(theta * r * k), imag[k]) for k in ks])

    out[0] = combine([(1.0, v) for v in real])
    out[mid] = cosines(mid, list(four) + list(two)) - sines(mid, odd)

    def place(r, cos_even, sin_even):
        cos_odd, sin_odd = cosines(r, odd), sines(r, odd)
        out[r] = (cos_even - sin_even) + (cos_odd - sin_odd)
        out[half - r] = (cos_even + sin_even) - (cos_odd + sin_odd)

    for r in range(1, quarter):
        c0, c2, s0, s2 = cosines(r, four), cosines(r, two), sines(r, four), sines(r, two)
        place(r, c0 + c2, s0 + s2)
        place(mid - r, c0 - c2, s2 - s0)
    place(quarter, cosines(quarter, four), sines(quarter, two))
    return out


GROUP = 16
REACH = 2
ROUNDS = 2
LANES = 128
CHUNK = 512


def layer_kernel(
    tokens_h, outer_h, inner_h, value_h, feats_h, output_h,
    taps_h, feature_weight_h, feature_phase_h, inner_mats_h, inner_phase_h, frequency_h, forward_h, backward_h,
    rate_h, skip_h, twist_h, trig_h,
    out_ref,
    tok, weights, outer_w, feats, output_w, taps, feature_weight, feature_phase, inner_mats, inner_phase, frequency,
    forward, backward, rate, skip, twist, trig,
    hid, sig_send, sig_recv, gs_send, gs_recv, resp_send, resp_recv,
    sums, diffs, turned, filt, back, scale_ref, first_ref, chan, rate_col, energy_ref, signal_ref, total_ref,
    edge_ref, edge_out, edge_in, end_ref,
    load_sem, small_sem, edge_send, edge_recv, hid_s, hid_r, sig_s, sig_r, gs_s, gs_r, resp_s, resp_r, alive,
):
    f32, bf16 = jnp.float32, jnp.bfloat16
    dot = functools.partial(jnp.dot, preferred_element_type=f32)
    n_row, n_col = lax.axis_size("row"), lax.axis_size("col")
    row, col = lax.axis_index("row"), lax.axis_index("col")
    rows, depth = tokens_h.shape
    length = rows * n_row
    half = feats.shape[0]
    width = outer_h.shape[1]
    count = width // n_row
    parts = count // GROUP
    wide = width // parts
    planes = length // WIDE
    per = rows // WIDE
    share = rows // n_col
    halves = width // LANES
    pair = parts // halves
    spec = (planes + 1) * GROUP
    mesh_id = pl.DeviceIdType.MESH

    def arrived(ref, semaphore):
        pltpu.make_async_copy(ref, ref, semaphore).wait()

    barrier = pltpu.get_barrier_semaphore()
    reach = REACH

    def along(step, semaphore):
        @pl.when(row >= step)
        def _():
            pl.semaphore_signal(semaphore, inc=1, device_id=(row - step, col), device_id_type=mesh_id)

        @pl.when(row < n_row - step)
        def _():
            pl.semaphore_signal(semaphore, inc=1, device_id=(row + step, col), device_id_type=mesh_id)

    def either(step):
        return jnp.where(row >= step, 1, 0) + jnp.where(row < n_row - step, 1, 0)

    for step in range(1, reach + 1):
        along(step, barrier)
    for o in range(1, n_col):
        pl.semaphore_signal(barrier, inc=1, device_id=(row, lax.rem(col + o, n_col)), device_id_type=mesh_id)
    side = lax.rem(col, 2)
    partner = col + 1 - 2 * side
    small = [
        pltpu.make_async_copy(source, target, small_sem.at[i])
        for i, (source, target) in enumerate([
            (feature_weight_h, feature_weight), (feature_phase_h, feature_phase), (inner_mats_h, inner_mats),
            (inner_phase_h, inner_phase), (frequency_h, frequency), (forward_h, forward), (backward_h, backward),
            (rate_h, rate), (taps_h, taps), (skip_h, skip), (twist_h, twist), (trig_h, trig)])
    ]
    feature_load = pltpu.make_async_copy(
        feats_h.at[pl.ds(pl.multiple_of(side * half, CHUNK), half)], feats, load_sem.at[0])
    first_load = pltpu.make_async_copy(tokens_h.at[0:16], tok.at[0:16], load_sem.at[1])
    last_load = pltpu.make_async_copy(tokens_h.at[rows - 16 : rows], tok.at[rows - 16 : rows], load_sem.at[1])
    token_load = pltpu.make_async_copy(tokens_h.at[16 : rows - 16], tok.at[16 : rows - 16], load_sem.at[2])
    weight_loads = [
        [
            pltpu.make_async_copy(
                source.at[:, h * LANES : (h + 1) * LANES], weights.at[h, :, j * LANES : (j + 1) * LANES],
                load_sem.at[3 + h])
            for j, source in enumerate((inner_h, value_h))
        ]
        for h in range(halves)
    ]
    base = 3 + halves
    outer_load = pltpu.make_async_copy(outer_h, outer_w, load_sem.at[base])
    output_loads = [
        pltpu.make_async_copy(
            output_h.at[c * width + h * wide : c * width + (h + 1) * wide],
            output_w.at[h, c * wide : (c + 1) * wide], load_sem.at[base + 1])
        for h in range(parts) for c in range(n_col)
    ]
    for copy in [first_load, last_load] + small[:5] + [feature_load, token_load]:
        copy.start()
    for copy in sum(weight_loads, []):
        copy.start()
    for copy in small[5:]:
        copy.start()

    arrived(tok.at[0:32], load_sem.at[1])
    ends = [tok[rows - 16 : rows].astype(f32)[15:16], tok[0:16].astype(f32)[0:1]]
    for j, end in enumerate(ends):
        for i in range(depth // LANES):
            edge_ref[j, i : i + 1, :] = end[:, i * LANES : (i + 1) * LANES]
        edge_out[j] = edge_ref[j].astype(bf16)
    pl.semaphore_wait(barrier, n_col - 1 + either(1) + either(2))
    down = pltpu.make_async_remote_copy(
        src_ref=edge_out.at[0], dst_ref=edge_in.at[0],
        send_sem=edge_send.at[0], recv_sem=edge_recv.at[0],
        device_id=(lax.rem(row + 1, n_row), col), device_id_type=mesh_id)
    up = pltpu.make_async_remote_copy(
        src_ref=edge_out.at[1], dst_ref=edge_in.at[1],
        send_sem=edge_send.at[1], recv_sem=edge_recv.at[1],
        device_id=(lax.rem(row + n_row - 1, n_row), col), device_id_type=mesh_id)

    @pl.when(row < n_row - 1)
    def _():
        down.start()

    @pl.when(row > 0)
    def _():
        up.start()

    along(reach, alive.at[0])
    known = 2 * reach
    rounds = 1

    for copy in small[:5]:
        copy.wait()
    turn = frequency[...] * (0.5 / math.pi)
    high, low = split_two(feature_weight[...] * turn)
    phase_high, phase_low = split_two(feature_phase[...] * turn)
    used = high.shape[0]
    first_ref[...] = jnp.zeros_like(first_ref)
    first_ref[0:used] = high.astype(f32)
    first_ref[40 : 40 + used] = high.astype(f32)
    first_ref[80 : 80 + used] = low.astype(f32)
    first_ref[120:121] = phase_high.astype(f32)
    first_ref[121:122] = phase_low.astype(f32)
    first_w = first_ref[...].astype(bf16)
    inner_w = []
    for level in range(INNER):
        mat_high, mat_low = split_two(inner_mats[level] * turn)
        inner_w.append(jnp.concatenate([
            jnp.concatenate([mat_high, mat_low], 1), jnp.concatenate([mat_high, jnp.zeros_like(mat_low)], 1)], 0))
    inner_p = inner_phase[...] * turn

    def hidden_chunk(i):
        at = pl.ds(i * CHUNK, CHUNK)
        hidden = sine_of_turns(dot(feats[at, :], first_w))
        for level in range(INNER):
            h_high, h_low = split_two(hidden)
            both = dot(jnp.concatenate([h_high, h_low], 1), inner_w[level])
            hidden = sine_of_turns(both[:, :LANES] + both[:, LANES:] + inner_p[level : level + 1, :])
        hid[side, at, :] = hidden.astype(bf16)

    pieces = half // CHUNK
    to_partner = []
    for i in range(pieces):
        part = hid.at[side, pl.ds(i * CHUNK, CHUNK)]
        to_partner.append(pltpu.make_async_remote_copy(
            src_ref=part, dst_ref=part, send_sem=hid_s.at[0], recv_sem=hid_r.at[0],
            device_id=(row, partner), device_id_type=mesh_id))

    feature_load.wait()
    for i in range(pieces - 1):
        hidden_chunk(i)
        to_partner[i].start()
    while known < n_row - 1:
        pl.semaphore_wait(alive.at[rounds - 1], either(known // 2))
        along(known, alive.at[rounds])
        known, rounds = 2 * known, rounds + 1
    token_load.wait()
    arrived(weights.at[0], load_sem.at[3])
    for copy in [outer_load] + output_loads:
        copy.start()
    index = lax.broadcasted_iota(jnp.int32, (rows, 2 * LANES), 0)

    def halved(matrix):
        return jnp.concatenate([dot(tok[: rows // 2], matrix), dot(tok[rows // 2 :], matrix)], 0)

    def edged(matrix):
        middle = depth // 2
        return dot(end_rows[:, :middle], matrix[:middle]) + dot(end_rows[:, middle:], matrix[middle:])

    def convolved(main, ends, tap):
        first = jnp.where(row > 0, ends[0:1], 0.0)
        last = jnp.where(row < n_row - 1, ends[1:2], 0.0)
        at_row = index[:, : main.shape[1]]
        before = jnp.where(at_row == 0, first, pltpu.roll(main, 1, 0))
        after = jnp.where(at_row == rows - 1, last, pltpu.roll(main, rows - 1, 0))
        return before * tap[0] + main * tap[1] + after * tap[2]

    def rounded(value):
        return value.astype(bf16).astype(f32)

    other = 1 - lax.div(row, n_row // 2)
    place = lax.rem(row, n_row // 2)
    peers = [other * (n_row // 2) + lax.rem(place + i, n_row // 2) for i in range(n_row // 2)]
    peers += [(1 - other) * (n_row // 2) + lax.rem(place + i, n_row // 2) for i in range(1, n_row // 2)]

    for copy in small[5:]:
        copy.wait()
    chan[0] = forward[...].T
    chan[1] = backward[...].T
    rate_col[...] = jnp.broadcast_to(rate[...], (LANES, width)).T
    mine = [pl.ds(pl.multiple_of(h * wide + row * GROUP, GROUP), GROUP) for h in range(parts)]
    both_w = jnp.concatenate([chan[j, own, :] for j in range(2) for own in mine], 0).astype(bf16)
    rates = jnp.concatenate([rate_col[own, 0:1] for own in mine], 0)
    energy_ref[...] = jnp.zeros_like(energy_ref)

    def gs_share(j, value):
        for p in range(n_col):
            gs_send[p, j] = value[:, p * share : (p + 1) * share]
        for o in range(1, n_col):
            peer = lax.rem(col + o, n_col)
            pltpu.make_async_remote_copy(
                src_ref=gs_send.at[peer, j], dst_ref=gs_recv.at[col, j],
                send_sem=gs_s.at[0], recv_sem=gs_r.at[0], device_id=(row, peer), device_id_type=mesh_id).start()
        gs_recv[col, j] = gs_send[col, j]

    for h in range(halves):
        if h > 0:
            arrived(weights.at[h], load_sem.at[3 + h])
        main = rounded(halved(weights[h]))
        if h == 0:
            @pl.when(row > 0)
            def _():
                down.wait_recv()

            @pl.when(row < n_row - 1)
            def _():
                up.wait_recv()

            pl.semaphore_wait(alive.at[rounds - 1], either(known // 2))
            for j in range(2):
                edge_ref[j] = edge_in[j].astype(f32)
                for i in range(depth // LANES):
                    end_ref[j : j + 1, i * LANES : (i + 1) * LANES] = edge_ref[j, i : i + 1, :]
            end_rows = end_ref[...].astype(bf16)
        ends = rounded(edged(weights[h]))
        at = slice(h * LANES, (h + 1) * LANES)
        tap = [jnp.concatenate([taps[i, 1:2, at], taps[i, 2:3, at]], 1) for i in range(3)]
        made = convolved(main, ends, tap)
        signal = (made[:, :LANES] * made[:, LANES:]).astype(bf16).astype(f32).T
        signal_ref[h] = signal
        flipped = signal.astype(bf16)
        for q in range(h * pair, (h + 1) * pair):
            for g in range(n_row):
                top = (q - h * pair) * wide + g * GROUP
                sig_send[q, g] = flipped[top : top + GROUP]
            for i, peer in enumerate(peers):
                pltpu.make_async_remote_copy(
                    src_ref=sig_send.at[q, peer], dst_ref=sig_recv.at[q, row],
                    send_sem=sig_s.at[0], recv_sem=sig_r.at[q],
                    device_id=(peer, col), device_id_type=mesh_id).start()
            sig_recv[q, row] = sig_send[q, row]

    skip_col = jnp.broadcast_to(skip[...], (LANES, width)).T
    direct = jnp.concatenate([signal_ref[h] * skip_col[h * LANES : (h + 1) * LANES, 0:1] for h in range(halves)], 0)
    gs_share(1, direct.astype(bf16))

    hidden_chunk(pieces - 1)
    to_partner[pieces - 1].start()
    outer_load.wait()
    main, ends = rounded(halved(outer_w[...])), rounded(edged(outer_w[...]))
    gate = rounded(convolved(main, ends, [taps[i, 0:1] for i in range(3)])).T.astype(bf16)
    gs_share(0, gate)

    def filter_chunk(owner, i):
        start = owner * half + i * CHUNK
        at = pl.ds(pl.multiple_of(start, CHUNK), CHUNK)
        both = lax.dot_general(both_w, hid[owner, pl.ds(i * CHUNK, CHUNK), :], (((1,), (1,)), ((), ())),
                               preferred_element_type=f32)
        place = lax.broadcasted_iota(jnp.int32, (count, CHUNK), 1) + start
        window = jnp.exp(place.astype(f32) * (-1.0 / (length - 1)) * rates)
        ahead = both[:count] * window
        behind = jnp.where(place == 0, 0.0, both[count:] * window)
        sums[:, at] = ahead + behind
        diffs[:, at] = ahead - behind
        energy_ref[...] += jnp.broadcast_to(
            jnp.sum(ahead * ahead + behind * behind, axis=1, keepdims=True), (count, LANES))

    for i in range(pieces):
        filter_chunk(side, i)
    arrived(hid.at[1 - side], hid_r.at[0])
    for i in range(pieces):
        filter_chunk(1 - side, i)
    scale_ref[...] = lax.rsqrt(1.0 + energy_ref[...]) * (0.5 / length)

    def turn_into(first, pairs, base_row, left, weighted):
        for k, (real, imag) in enumerate(pairs):
            c, s = twist[0, k : k + 1, pl.ds(left, LANES)], twist[1, k : k + 1, pl.ds(left, LANES)]
            if weighted and k not in (0, planes):
                c, s = c * 2.0, s * 2.0
            at = pl.ds(pl.multiple_of(base_row + k * GROUP, GROUP), GROUP)
            if imag is None:
                new_real, new_imag = real * c, -(real * s)
            else:
                new_real, new_imag = real * c + imag * s, imag * c - real * s
            turned[first, at, pl.ds(left, LANES)] = new_real.astype(bf16)
            turned[first, at, pl.ds(pl.multiple_of(WIDE + left, LANES), LANES)] = new_imag.astype(bf16)

    lanes = WIDE // LANES

    def filter_tile(i, carry):
        h, left = i // lanes, pl.multiple_of(i % lanes * LANES, LANES)
        top = pl.ds(pl.multiple_of(h * GROUP, GROUP), GROUP)
        scale = scale_ref[top, :]
        for which, source in enumerate((sums, diffs)):
            got = [source[top, pl.ds(pl.multiple_of(r * WIDE + left, LANES), LANES)] * scale for r in range(planes)]
            turn_into(which, first_stage(got), h * spec, left, True)
        return carry

    lax.fori_loop(0, parts * lanes, filter_tile, 0)
    filt[0] = dot(turned[0], trig[:, :WIDE])
    filt[1] = dot(turned[1], trig[:, WIDE:])

    for h in range(parts):
        arrived(sig_recv.at[h, pl.ds(0, n_row - 1)], sig_r.at[h])
        band = pl.ds(h * spec, spec)

        def signal_tile(i, carry):
            left = pl.multiple_of(i * LANES, LANES)
            got = [sig_recv[h, r // per, :, pl.ds(pl.multiple_of(r % per * WIDE + left, LANES), LANES)].astype(f32)
                   for r in range(planes)]
            turn_into(0, first_stage(got), h * spec, left, False)
            return carry

        lax.fori_loop(0, lanes, signal_tile, 0)
        spectrum = dot(turned[0, band], trig[...])
        real, imag = spectrum[:, :WIDE], spectrum[:, WIDE:]
        prod_real = (real * filt[0, band] - imag * filt[1, band]).astype(bf16)
        prod_imag = (real * filt[1, band] + imag * filt[0, band]).astype(bf16)
        back[...] = dot(jnp.concatenate([prod_imag, prod_real], 1), trig[...])

        def back_tile(i, carry):
            left = pl.multiple_of(i * LANES, LANES)
            pairs = []
            for k in range(planes + 1):
                c, s = twist[0, k : k + 1, pl.ds(left, LANES)], twist[1, k : k + 1, pl.ds(left, LANES)]
                at = pl.ds(k * GROUP, GROUP)
                b_imag, b_real = back[at, pl.ds(left, LANES)], back[at, pl.ds(pl.multiple_of(WIDE + left, LANES), LANES)]
                pairs.append((b_real * c - b_imag * s, b_imag * c + b_real * s))
            for r, plane in enumerate(last_stage(pairs)):
                resp_send[h, r // per, r % per * lanes + i] = plane.astype(bf16)
            return carry

        lax.fori_loop(0, lanes, back_tile, 0)
        for i, peer in enumerate(peers + [row]):
            for o in range(n_col):
                if i == n_row - 1 and o == 0:
                    continue
                target = lax.rem(col + o, n_col)
                pltpu.make_async_remote_copy(
                    src_ref=resp_send.at[h, peer, target], dst_ref=resp_recv.at[h, col, row],
                    send_sem=resp_s.at[0], recv_sem=resp_r.at[h],
                    device_id=(peer, target), device_id_type=mesh_id).start()
        resp_recv[h, col, row] = resp_send[h, row, col]

    arrived(gs_recv.at[pl.ds(0, n_col - 1)], gs_r.at[0])
    arrived(output_w, load_sem.at[base + 1])
    for h in range(parts):
        arrived(resp_recv.at[h].reshape(n_row * n_col, GROUP, share).at[pl.ds(0, n_row * n_col - 1)], resp_r.at[h])
        shape = (n_col * wide, share)
        response = resp_recv[h].reshape(shape).astype(f32)
        gate, direct = (gs_recv[:, j, h * wide : (h + 1) * wide].reshape(shape).astype(f32) for j in range(2))
        mixed = (gate * (response + direct)).T.astype(bf16)
        got = dot(mixed, output_w[h])
        if h == 0:
            total_ref[...] = got
        elif h < parts - 1:
            total_ref[...] += got
        else:
            out_ref[...] = (total_ref[...] + got).astype(bf16)

    @pl.when(row < n_row - 1)
    def _():
        down.wait_send()

    @pl.when(row > 0)
    def _():
        up.wait_send()

    arrived(hid.at[side], hid_s.at[0])
    arrived(sig_send.at[:, pl.ds(0, n_row - 1)], sig_s.at[0])
    arrived(gs_send.at[pl.ds(0, n_col - 1)], gs_s.at[0])
    arrived(resp_send.reshape(parts, n_row * n_col, GROUP, share).at[:, pl.ds(0, n_row * n_col - 1)], resp_s.at[0])


def fits(tokens_rows, seq_length, own_width, row_devices, col_devices, units):
    planes = seq_length // WIDE
    members = own_width // row_devices
    return (
        members % (2 * GROUP) == 0
        and own_width % row_devices == 0
        and LANES % (row_devices * GROUP) == 0
        and own_width % LANES == 0
        and row_devices <= REACH * 2 ** ROUNDS
        and row_devices > REACH * 2 ** (ROUNDS - 1)
        and row_devices % 2 == 0
        and tokens_rows % WIDE == 0
        and planes % 8 == 0
        and 8 <= planes <= 32
        and units == LANES
        and col_devices == 4
        and tokens_rows == col_devices * LANES
        and seq_length % (4 * CHUNK) == 0
    )


def on_device_fast(
    tokens, outer_weight, inner_weight, value_weight, conv_taps, feature_weight, feature_phase,
    inner_mats, inner_phase, frequency, forward_weight, backward_weight, decay_rate, skip_gain, output_weight,
):
    f32, bf16 = jnp.float32, jnp.bfloat16
    rows, depth = tokens.shape
    devices = lax.axis_size("row")
    seq_length = rows * devices
    width = outer_weight.shape[1]
    members = width // devices
    parts = members // GROUP
    wide = width // parts
    halves = width // LANES
    planes = seq_length // WIDE
    n_col = lax.axis_size("col")
    k_index = np.arange(planes + 1)[:, None] * np.arange(WIDE)[None, :]
    twist_angle = 2 * np.pi * k_index / (2 * seq_length)
    twist = jnp.asarray(np.stack([np.cos(twist_angle), np.sin(twist_angle)]), f32)
    w_angle = 2 * np.pi * (np.arange(WIDE)[:, None] * np.arange(WIDE)[None, :] % WIDE) / WIDE
    cos_w, sin_w = np.cos(w_angle), np.sin(w_angle)
    trig = jnp.asarray(np.block([[cos_w, -sin_w], [sin_w, cos_w]]), bf16)
    spec = (planes + 1) * GROUP
    any_spec = pl.BlockSpec(memory_space=pl.ANY)
    dma = pltpu.SemaphoreType.DMA
    share = rows // n_col
    half = seq_length // 2
    pieces = half // CHUNK
    small = [
        conv_taps, feature_weight, feature_phase[None], inner_mats, inner_phase, frequency[None],
        forward_weight, backward_weight, decay_rate[None], skip_gain[None], twist, trig]
    exchanged = pltpu.VMEM((parts, devices, GROUP, rows), bf16)
    spread = pltpu.VMEM((n_col, 2, width, share), bf16)
    return pl.pallas_call(
        layer_kernel,
        out_shape=pltpu.VMEM((share, output_weight.shape[1]), bf16),
        in_specs=[any_spec] * (6 + len(small)),
        out_specs=pl.BlockSpec(memory_space=pltpu.VMEM),
        scratch_shapes=[
            pltpu.VMEM((rows, depth), bf16),
            pltpu.VMEM((halves, depth, 2 * LANES), bf16),
            pltpu.VMEM((depth, width), bf16),
            pltpu.VMEM((half, LANES), bf16),
            pltpu.VMEM((parts, n_col * wide, output_weight.shape[1]), bf16),
        ] + [pltpu.VMEM(a.shape, a.dtype) for a in small] + [
            pltpu.VMEM((2, half, LANES), bf16),
            exchanged, exchanged, spread, spread,
            pltpu.VMEM((parts, devices, n_col, GROUP, share), bf16),
            pltpu.VMEM((parts, n_col, devices, GROUP, share), bf16),
            pltpu.VMEM((members, seq_length), f32),
            pltpu.VMEM((members, seq_length), f32),
            pltpu.VMEM((2, parts * spec, 2 * WIDE), bf16),
            pltpu.VMEM((2, parts * spec, WIDE), f32),
            pltpu.VMEM((spec, 2 * WIDE), f32),
            pltpu.VMEM((members, LANES), f32),
            pltpu.VMEM((LANES, LANES), f32),
            pltpu.VMEM((2, width, LANES), f32),
            pltpu.VMEM((width, LANES), f32),
            pltpu.VMEM((members, LANES), f32),
            pltpu.VMEM((halves, LANES, rows), f32),
            pltpu.VMEM((share, output_weight.shape[1]), f32),
            pltpu.VMEM((2, depth // LANES, LANES), f32),
            pltpu.VMEM((2, depth // LANES, LANES), bf16),
            pltpu.VMEM((2, depth // LANES, LANES), bf16),
            pltpu.VMEM((16, depth), f32),
            dma((5 + halves,)), dma((len(small),)), dma((2,)), dma((2,)), dma((1,)), dma((1,)),
            dma((1,)), dma((parts,)), dma((1,)), dma((1,)), dma((1,)), dma((parts,)),
            pltpu.SemaphoreType.REGULAR((ROUNDS,)),
        ],
        compiler_params=pltpu.CompilerParams(
            collective_id=0, has_side_effects=True, vmem_limit_bytes=GRANT),
        name="layer",
    )(tokens, outer_weight, inner_weight, value_weight, jnp.asarray(feature_table(seq_length)), output_weight, *small)


GRANT = 58 * 1024 * 1024


def on_any(*args):
    tokens, outer_weight, feature_weight = args[0], args[1], args[5]
    devices = lax.axis_size("row")
    if fits(tokens.shape[0], tokens.shape[0] * devices, outer_weight.shape[1], devices, lax.axis_size("col"), feature_weight.shape[1]):
        return on_device_fast(*args)
    return on_device(*args)


def solution(mesh):
    placed = (
        P("row", None),
        P(None, "col"),
        P(None, "col"),
        P(None, "col"),
        P(None, None, "col"),
        P(),
        P(),
        P(),
        P(),
        P(),
        P(None, "col"),
        P(None, "col"),
        P("col"),
        P("col"),
        P(),
    )
    return jax.shard_map(
        on_any, mesh=mesh, in_specs=placed, out_specs=P(("row", "col"), None), check_vma=False
    )
```
